32 devices in a mesh: sp: 16 (over z, y, core), tp: 2 (over x).
Axes of the slice: x: 2, y: 2, z: 4, core: 2. Of those that a mesh axis runs over, the one named last changes fastest.
Arguments:
- activations: bfloat16 [4096, 2048], P('sp', 'tp'), may hold values from -8 to 8
- norm_gain: float32 [2048], replicated, may hold values from 0.1 to 1.9
- win_query: bfloat16 [2048, 1024], P(None, 'tp'), may hold values from -1 to 1
- win_key: bfloat16 [2048, 512], P(None, 'tp'), may hold values from -1 to 1
- win_value: bfloat16 [2048, 512], P(None, 'tp'), may hold values from -0.125 to 0.125
- sink_logit: float32 [16], P('tp'), may hold values from 1 to 6
- lat_query: bfloat16 [2048, 1536], P(None, 'tp'), may hold values from -1 to 1
- key_value_down_weight: bfloat16 [2048, 128], replicated, may hold values from -0.125 to 0.125
- rope_key: bfloat16 [2048, 64], replicated, may hold values from -1 to 1
- latent_norm_gain: float32 [128], replicated, may hold values from 0.1 to 1.9
- key_up_weight: bfloat16 [128, 1024], P(None, 'tp'), may hold values from -0.5 to 0.5
- value_up_weight: bfloat16 [128, 1024], P(None, 'tp'), may hold values from -0.5 to 0.5
- out_win: bfloat16 [1024, 2048], P('tp'), may hold values from -0.359375 to 0.359375
- out_lat: bfloat16 [1024, 2048], P('tp'), may hold values from -0.59765625 to 0.59765625
Outputs:
- mixed: bfloat16 [4096, 2048], P('sp', 'tp')
The draws below stay inside these ranges and needn't reach their ends.
All inputs are finite; a program needn't handle non-finite values.
Results may differ from the reference program's by a relative error of at most 0.025.
Values may be sent and summed in bfloat16 or wider, within the bound.
A program may use at most 64 MiB of HBM per device.

```python
import jax
import jax.numpy as jnp
from jax import lax

MODEL_WIDTH = 2048
HEADS_A = 16
KV_A = 8
DH = 64
WINDOW = 128
LATENT_HEADS = 8
LATENT_WIDTH = 128
UNROTATED_WIDTH = 128
D_ROPE = 64
VALUE_WIDTH = 128
TOK_DEV = 256
SEQ = 4096


def drawn(key, row_count, col_count, spread):
    values = jnp.clip(jax.random.normal(key, (row_count, col_count), jnp.float32) * spread, -1.0, 1.0)
    return values.astype(jnp.bfloat16)


def draw_activations(key, part):
    key_base = jax.random.fold_in(key, 11)
    values = jnp.clip(jax.random.normal(key_base, (SEQ, MODEL_WIDTH), jnp.float32), -6.0, 6.0)
    return values.astype(jnp.bfloat16)


def draw_win_query(key, part):
    return drawn(jax.random.fold_in(key, 21), MODEL_WIDTH, HEADS_A * DH, MODEL_WIDTH ** (-0.5))


def draw_win_key(key, part):
    return drawn(jax.random.fold_in(key, 22), MODEL_WIDTH, KV_A * DH, MODEL_WIDTH ** (-0.5))


def draw_lat_query(key, part):
    return drawn(jax.random.fold_in(key, 23), MODEL_WIDTH, LATENT_HEADS * (UNROTATED_WIDTH + D_ROPE), 2.5 * MODEL_WIDTH ** (-0.5))


def draw_rope_key(key, part):
    return drawn(jax.random.fold_in(key, 24), MODEL_WIDTH, D_ROPE, MODEL_WIDTH ** (-0.5))


def levels(stream_key, shape, split, least, largest):
    gain, own = 1.0, jax.random.fold_in(stream_key, 6)
    for position, shards_of in split:
        heights = jnp.exp(jax.random.uniform(jax.random.fold_in(own, position), (shards_of,), jnp.float32, least / len(split), largest / len(split)))
        gain = gain * jnp.repeat(heights, shape[position] // shards_of).reshape([-1 if axis == position else 1 for axis in range(len(shape))])
    return gain


def bell_draw(own_key, dims, scale, bound, shards=(), kind=jnp.bfloat16):
    result = jax.random.normal(own_key, dims, jnp.float32) * scale
    if len(shards) > 0:
        result = levels(own_key, dims, shards, -0.22, 0.18) * result
    return jnp.clip(result, min=-bound, max=bound).astype(kind)


def setup_inputs(seed: int = 0) -> dict:
    key_of = jax.random.split(jax.random.key(seed), 15)
    return {
        "activations": draw_activations(jax.random.fold_in(key_of[14], 71), 0),
        "norm_gain": jnp.clip(1.0 + 0.18 * jax.random.normal(key_of[1], (MODEL_WIDTH,), jnp.float32), 0.1, 1.9),
        "win_query": draw_win_query(jax.random.fold_in(key_of[14], 71), 0),
        "win_key": draw_win_key(jax.random.fold_in(key_of[14], 71), 0),
        "win_value": bell_draw(key_of[4], (MODEL_WIDTH, KV_A * DH), MODEL_WIDTH ** -0.5, 0.125, ((1, 2),)),
        "sink_logit": jnp.clip(1.0 + 5.0 * jax.random.uniform(key_of[5], (HEADS_A,), jnp.float32) ** levels(key_of[5], (HEADS_A,), ((0, 2),), -0.2, 0.2), 1.0, 6.0),
        "lat_query": draw_lat_query(jax.random.fold_in(key_of[14], 71), 0),
        "key_value_down_weight": bell_draw(key_of[7], (MODEL_WIDTH, LATENT_WIDTH), MODEL_WIDTH ** -0.5, 0.125),
        "rope_key": draw_rope_key(jax.random.fold_in(key_of[14], 71), 0),
        "latent_norm_gain": jnp.clip(1.0 + 0.18 * jax.random.normal(key_of[9], (LATENT_WIDTH,), jnp.float32), 0.1, 1.9),
        "key_up_weight": bell_draw(key_of[10], (LATENT_WIDTH, LATENT_HEADS * UNROTATED_WIDTH), LATENT_WIDTH ** -0.5, 0.5, ((1, 2),)),
        "value_up_weight": bell_draw(key_of[11], (LATENT_WIDTH, LATENT_HEADS * VALUE_WIDTH), LATENT_WIDTH ** -0.5, 0.5, ((1, 2),)),
        "out_win": bell_draw(key_of[12], (HEADS_A * DH, MODEL_WIDTH), 0.06, 0.359375, ((0, 2),)),
        "out_lat": bell_draw(key_of[13], (LATENT_HEADS * VALUE_WIDTH, MODEL_WIDTH), 0.1, 0.59765625, ((0, 2),)),
    }


EPSILON = 1e-06
ROPE_BASE = 10000.0

def rotate(vectors, angles):
    half_width = vectors.shape[-1] // 2
    cosine_table = jnp.cos(angles)
    sine_table = jnp.sin(angles)
    lower_half = vectors[..., :half_width]
    upper_half = vectors[..., half_width:]
    return jnp.concatenate([lower_half * cosine_table - upper_half * sine_table, lower_half * sine_table + upper_half * cosine_table], axis=-1)

def rotary_angles(places, width):
    frequency = 1.0 / ROPE_BASE ** (jnp.arange(0, width, 2).astype(jnp.float32) / width)
    return places[:, None] * frequency[None, :]

def reference(activations, norm_gain, win_query, win_key, win_value, sink_logit, lat_query, key_value_down_weight, rope_key, latent_norm_gain, key_up_weight, value_up_weight, out_win, out_lat):
    widened = activations.astype(jnp.float32)
    row_scale = lax.rsqrt(lax.optimization_barrier(jnp.mean(widened * widened, axis=1)) + EPSILON)[:, None]
    normalized = (widened * norm_gain[None, :]).astype(jnp.bfloat16)

    def project(weight):
        return jnp.dot(normalized, weight, preferred_element_type=jnp.float32)
    win_queries = (project(win_query) * row_scale).astype(jnp.bfloat16)
    win_keys = (project(win_key) * row_scale).astype(jnp.bfloat16)
    win_values = (project(win_value) * row_scale).astype(jnp.bfloat16)
    places = jnp.arange(SEQ).astype(jnp.float32)
    angles = rotary_angles(places, D_ROPE)
    query_all = (project(lat_query) * row_scale).reshape(SEQ, LATENT_HEADS, UNROTATED_WIDTH + D_ROPE)
    query_plain = query_all[..., :UNROTATED_WIDTH].astype(jnp.bfloat16)
    query_turned = rotate(query_all[..., UNROTATED_WIDTH:], angles[:, None, :]).astype(jnp.bfloat16)
    compressed = project(key_value_down_weight)
    latent = (compressed * lax.rsqrt(lax.optimization_barrier(jnp.mean(compressed * compressed, axis=1, keepdims=True)) + EPSILON) * latent_norm_gain[None, :]).astype(jnp.bfloat16)
    key_rotary = rotate(project(rope_key) * row_scale, angles).astype(jnp.bfloat16)
    key_nope = jnp.dot(latent, key_up_weight, preferred_element_type=jnp.float32).astype(jnp.bfloat16)
    value_lat = jnp.dot(latent, value_up_weight, preferred_element_type=jnp.float32).astype(jnp.bfloat16)
    block_count = SEQ // WINDOW
    groups = HEADS_A // KV_A
    query_blocks = win_queries.reshape(block_count, WINDOW, KV_A, groups, DH)
    zero_rim = jnp.zeros((WINDOW, KV_A * DH), jnp.bfloat16)
    key_padded = jnp.concatenate([zero_rim, win_keys, zero_rim], 0).reshape(block_count + 2, WINDOW, KV_A, DH)
    value_padded = jnp.concatenate([zero_rim, win_values, zero_rim], 0).reshape(block_count + 2, WINDOW, KV_A, DH)
    key_near = jnp.concatenate([key_padded[:-2], key_padded[1:-1], key_padded[2:]], axis=1)
    value_near = jnp.concatenate([value_padded[:-2], value_padded[1:-1], value_padded[2:]], axis=1)
    slopes = jnp.exp2(-8.0 * jnp.arange(1, HEADS_A + 1).astype(jnp.float32) / HEADS_A).reshape(KV_A, groups)
    sink_table = sink_logit.reshape(KV_A, groups)

    def window_block(inputs):
        query_block, key_block, value_block, block_index = inputs
        query_pos = block_index * WINDOW + jnp.arange(WINDOW, dtype=jnp.int32)
        key_pos = (block_index - 1) * WINDOW + jnp.arange(3 * WINDOW, dtype=jnp.int32)
        distance = jnp.abs(query_pos[:, None] - key_pos[None, :])
        in_window = (distance <= WINDOW) & (key_pos[None, :] >= 0) & (key_pos[None, :] < SEQ)
        scores = jnp.einsum('qhgd,khd->hgqk', query_block.astype(jnp.float32), key_block.astype(jnp.float32)) * DH ** (-0.5)
        scores = scores - slopes[:, :, None, None] * distance.astype(jnp.float32)[None, None]
        scores = jnp.where(in_window[None, None], scores, -jnp.inf)
        row_peak = jnp.maximum(lax.optimization_barrier(jnp.max(scores, axis=3)), sink_table[:, :, None])
        weights = jnp.exp(scores - row_peak[..., None])
        denominator = lax.optimization_barrier(jnp.sum(weights, axis=3)) + jnp.exp(sink_table[:, :, None] - row_peak)
        rounded = lax.optimization_barrier(weights.astype(jnp.bfloat16)).astype(jnp.float32)
        blended = jnp.einsum('hgqk,khd->qhgd', rounded, value_block.astype(jnp.float32))
        blended = blended / jnp.transpose(denominator, (2, 0, 1))[..., None]
        return blended.reshape(WINDOW, HEADS_A * DH).astype(jnp.bfloat16)
    win_out = lax.map(window_block, (query_blocks, key_near, value_near, jnp.arange(block_count, dtype=jnp.int32))).reshape(SEQ, HEADS_A * DH)
    span_count = SEQ // TOK_DEV
    plain_keys = key_nope.astype(jnp.float32).reshape(SEQ, LATENT_HEADS, UNROTATED_WIDTH)
    lat_values = value_lat.astype(jnp.float32).reshape(SEQ, LATENT_HEADS, VALUE_WIDTH)
    turned_keys = key_rotary.astype(jnp.float32)

    def latent_block(inputs):
        plain_block, turned_block = inputs
        scores = (jnp.einsum('qhd,khd->hqk', plain_block.astype(jnp.float32), plain_keys) + jnp.einsum('qhd,kd->hqk', turned_block.astype(jnp.float32), turned_keys)) * (UNROTATED_WIDTH + D_ROPE) ** (-0.5)
        row_peak = lax.optimization_barrier(jnp.max(scores, axis=2, keepdims=True))
        weights = jnp.exp(scores - row_peak)
        totals = lax.optimization_barrier(jnp.sum(weights, axis=2))
        rounded = lax.optimization_barrier(weights.astype(jnp.bfloat16)).astype(jnp.float32)
        blended = jnp.einsum('hqk,khd->qhd', rounded, lat_values) / jnp.transpose(totals)[..., None]
        return blended.reshape(TOK_DEV, LATENT_HEADS * VALUE_WIDTH).astype(jnp.bfloat16)
    lat_out = lax.map(latent_block, (query_plain.reshape(span_count, TOK_DEV, LATENT_HEADS, UNROTATED_WIDTH), query_turned.reshape(span_count, TOK_DEV, LATENT_HEADS, D_ROPE))).reshape(SEQ, LATENT_HEADS * VALUE_WIDTH)
    summed = jnp.dot(win_out, out_win, preferred_element_type=jnp.float32) + jnp.dot(lat_out, out_lat, preferred_element_type=jnp.float32)
    return summed.astype(jnp.bfloat16)
```

```python
import functools

import jax
import jax.numpy as jnp
import numpy as np
from jax import lax
from jax.experimental import pallas as pl
from jax.experimental.pallas import tpu as pltpu
from jax.sharding import PartitionSpec as P

HEADS_A = 16
DH = 64
WINDOW = 128
UNROTATED_WIDTH = 128
D_ROPE = 64
VALUE_WIDTH = 128

EPSILON = 1e-06
ROPE_BASE = 10000.0
LOG2E = 1.4426950408889634
MESH = pl.DeviceIdType.MESH
F32 = jnp.float32
BF16 = jnp.bfloat16
LEAD = 32
ONES = 16


def turn(vectors, cosine, sine):
    half = vectors.shape[-1] // 2
    swapped = jnp.concatenate([vectors[:, half:], vectors[:, :half]], axis=1)
    return vectors * cosine + swapped * sine


def dot_nt(a, b):
    return lax.dot_general(a, b, (((1,), (1,)), ((), ())), preferred_element_type=F32)


def dot(a, b):
    return jnp.dot(a, b, preferred_element_type=F32)


def remote(src, dst, send, recv, device):
    return pltpu.make_async_remote_copy(
        src_ref=src, dst_ref=dst, send_sem=send, recv_sem=recv, device_id=device, device_id_type=MESH
    )


def layer_kernel(
    n_sp, n_tp, parts,
    sink_ref,
    x_hbm, gain_hbm, near_hbm, base_hbm, lng_hbm, kup_hbm, vup_hbm,
    wkv_hbm, wr_hbm, wk_hbm, wv_hbm, wq_hbm, wlq_hbm, ow_hbm, ol_hbm,
    own_out, inc_out,
    xv, gain, near, base, lng, kup, vup, wkv, wr, wk, wv, wq, wlq, ow, ol,
    xn, xr, xm, ak, av, aq, alq, akv, ar, scale_ref, cs, ssq_out, ssq_in, pk_out, pk_in,
    gath, latt, qs, qwin, halo, acct, peaks, win, lat, outgoing, own,
    w_sem, x_send, x_recv, s_send, s_recv, p_send, p_recv, z_send, z_recv, y_send, y_recv,
    c_send, c_recv, h_send, h_recv, o_send, o_recv, f_sem,
):
    sp = lax.axis_index("sp")
    tp = lax.axis_index("tp")
    rows, local = xv.shape
    hi = n_sp // 4
    z, y, c = sp // 4, (sp // 2) % 2, sp % 2
    sub = rows // parts
    half = sub // 2
    heads = acct.shape[2] // WINDOW
    k_cols = ak.shape[1]
    cols = own.shape[2]

    def at(zz, yy, cc):
        return (zz * 2 + yy) * 2 + cc

    right, left = (sp + 1) % n_sp, (sp + n_sp - 1) % n_sp
    others = [(s, (tp + s) % n_tp) for s in range(1, n_tp)]
    sources = [(s, (tp + n_tp - s) % n_tp) for s in range(1, n_tp)]

    pairs = (
        (x_hbm, xv), (wkv_hbm, wkv), (wr_hbm, wr), (gain_hbm, gain),
        (near_hbm, near), (base_hbm, base), (lng_hbm, lng),
        (wk_hbm, wk), (wv_hbm, wv), (wq_hbm, wq), (wlq_hbm, wlq),
        (kup_hbm, kup), (vup_hbm, vup), (ow_hbm, ow), (ol_hbm, ol),
    )
    loads = [pltpu.make_async_copy(a, b, w_sem.at[i]) for i, (a, b) in enumerate(pairs)]
    for load in loads[:4]:
        load.start()

    barrier = pltpu.get_barrier_semaphore()
    peers = [(sp, other) for _, other in others]
    peers += [(at((z + d) % hi, y, c), tp) for d in range(1, hi)]
    peers += [(at(z, 1 - y, c), tp), (at(z, y, 1 - c), tp), (right, tp), (left, tp)]
    for peer in peers:
        pl.semaphore_signal(barrier, inc=1, device_id=peer, device_id_type=MESH)
    for load in loads[4:7]:
        load.start()
    latt[UNROTATED_WIDTH:, :] = jnp.ones_like(latt[UNROTATED_WIDTH:, :])
    for load in loads[:4]:
        load.wait()
    for load in loads[7:]:
        load.start()
    pl.semaphore_wait(barrier, len(peers))

    block_at = [(1 - c) * WINDOW, c * WINDOW]
    chunks = [(0, 0, LEAD), (0, LEAD, WINDOW - LEAD), (1, 0, WINDOW)]
    x_copies = {}
    for i, (block, start, size) in enumerate(chunks):
        where = pl.ds(pl.multiple_of(block_at[block] + start, LEAD), size)
        for s, other in others:
            x_copies[s, i] = remote(
                xv.at[where], xr.at[s - 1, where], x_send.at[s, i], x_recv.at[s, i], (sp, other)
            )
    for s, _ in others:
        x_copies[s, 0].start()

    mine = pl.ds(pl.multiple_of(tp * local, local), local)
    wide = xv[...].astype(F32)
    total = jnp.sum(wide * wide, axis=1, keepdims=True)
    ssq_out[...] = jnp.transpose(jnp.broadcast_to(total, (rows, 128)))[0:8]
    xn[...] = (wide * gain[tp]).astype(BF16)
    s_copies = [
        remote(ssq_out, ssq_in.at[s - 1], s_send.at[s], s_recv.at[s], (sp, other)) for s, other in others
    ]
    for copy in s_copies:
        copy.start()
    p_copies = {}
    for g in range(parts):
        span = slice(g * sub, (g + 1) * sub)
        comp = dot(xn[span], wkv[mine, :])
        turned = dot_nt(xn[span], wr[:, mine])
        akv[span] = comp
        ar[span] = turned
        pk_out[g, 0:sub] = comp.astype(BF16)
        pk_out[g, sub:] = jnp.concatenate([turned[:half], turned[half:]], axis=1).astype(BF16)
        for s, other in others:
            p_copies[s, g] = remote(
                pk_out.at[g], pk_in.at[s - 1, g], p_send.at[s, g], p_recv.at[s, g], (sp, other)
            )
            p_copies[s, g].start()
    for i in range(1, len(chunks)):
        for s, _ in others:
            x_copies[s, i].start()

    for load in loads[4:7]:
        load.wait()
    near_cos, near_sin = near[0], near[1]
    base_cos, base_sin = base[sp, 0:1, :], base[sp, 1:2, :]
    plain_sine = near_sin * base_cos + near_cos * base_sin
    lane = lax.broadcasted_iota(jnp.int32, plain_sine.shape, 1)
    cs[0] = near_cos * base_cos - near_sin * base_sin
    cs[1] = jnp.where(lane < D_ROPE // 2, -plain_sine, plain_sine)

    big = ((wk, ak), (wv, av), (wq, aq), (wlq, alq))
    for load, (weight, acc) in zip(loads[7:11], big):
        load.wait()
        acc[...] = dot(xn[...], weight[mine, :])

    relayed = hi == 4
    inner = (z + 1) % 4 >= 2
    if relayed:
        far = 2 - z // 2
        z_of = [z, z + 1 - 2 * (z % 2), far, 3 * (1 - z // 2)]
        z_to = {1: z_of[1], 2: far}
    else:
        z_of = [(z + hi - d) % hi for d in range(hi)]
        z_to = {d: (z + d) % hi for d in range(1, hi)}
    to_y, to_c = (at(z, 1 - y, c), tp), (at(z, y, 1 - c), tp)
    sends = []

    def forward(block, g, send, recv, device):
        copy = remote(gath.at[block, g], gath.at[block, g], send, recv, device)
        copy.start()
        return copy

    def block_of(d, dy, dc):
        return at(z_of[d], 1 - y if dy else y, 1 - c if dc else c)

    def to_core(d, dy, g):
        k = d + hi * dy
        sends.append(forward(block_of(d, dy, 0), g, c_send.at[k, g], c_recv.at[k, g], to_c))

    def to_row(d, g):
        sends.append(forward(block_of(d, 0, 0), g, y_send.at[d, g], y_recv.at[d, g], to_y))

    relays = []

    def got_z(d, g):
        block = block_of(d, 0, 0)
        origin = z_of[d]
        remote(
            gath.at[block, g], gath.at[block, g], z_send.at[d, g], z_recv.at[origin, g], to_y
        ).wait_recv()
        if relayed and d >= 2:
            copy = remote(
                gath.at[block, g], gath.at[block, g], z_send.at[(0, 3)[d - 2], g], z_recv.at[origin, g],
                (at(z_of[1], y, c), tp),
            )
            relays.append(copy)

            @pl.when(inner)
            def _():
                copy.start()
        to_row(d, g)
        to_core(d, 0, g)

    def got_y(d, g):
        block = block_of(d, 1, 0)
        remote(gath.at[block, g], gath.at[block, g], y_send.at[d, g], y_recv.at[d, g], to_y).wait_recv()
        to_core(d, 1, g)

    def got_c(d):
        for dy in range(2):
            for g in range(parts):
                block, k = block_of(d, dy, 1), d + hi * dy
                remote(gath.at[block, g], gath.at[block, g], c_send.at[k, g], c_recv.at[k, g], to_c).wait_recv()

    for copy in s_copies:
        copy.wait_recv()
    total = ssq_out[...]
    for s, _ in sources:
        total = total + ssq_in[s - 1]
    factor = lax.rsqrt(total / (local * n_tp) + EPSILON)
    scale_ref[...] = jnp.transpose(jnp.broadcast_to(factor[0:1], (128, rows)))
    for g in range(parts):
        span = slice(g * sub, (g + 1) * sub)
        comp = akv[span]
        turned = ar[span]
        for s, _ in sources:
            p_copies[s, g].wait_recv()
            comp = comp + pk_in[s - 1, g, 0:sub].astype(F32)
            both = pk_in[s - 1, g, sub:].astype(F32)
            turned = turned + jnp.concatenate([both[:, :D_ROPE], both[:, D_ROPE:]], axis=0)
        latent = comp * lax.rsqrt(jnp.mean(comp * comp, axis=1, keepdims=True) + EPSILON) * lng[...]
        turned = turn(turned * scale_ref[span, 0:D_ROPE], cs[0, span], cs[1, span])
        gath[sp, g, 0:sub] = latent.astype(BF16)
        gath[sp, g, sub:] = jnp.concatenate([turned[:half], turned[half:]], axis=1).astype(BF16)
        for d, zz in z_to.items():
            sends.append(forward(sp, g, z_send.at[d, g], z_recv.at[z, g], (at(zz, y, c), tp)))
        to_row(0, g)
        to_core(0, 0, g)

    def widen(scale, width):
        return jnp.concatenate([scale] * (-(-width // 128)), axis=1)[:, :width]

    def arrive(index):
        for i, (block, _, _) in enumerate(chunks):
            if block == index:
                for s, _ in others:
                    x_copies[s, i].wait_recv()
        where = pl.ds(pl.multiple_of(block_at[index], WINDOW), WINDOW)
        for s, source in sources:
            xm[s - 1] = (xr[s - 1, where, :].astype(F32) * gain[source]).astype(BF16)

    def finish(index, weight, acc):
        where = pl.ds(pl.multiple_of(block_at[index], WINDOW), WINDOW)
        result = acc[where, :]
        for s, source in sources:
            theirs = pl.ds(pl.multiple_of(source * local, local), local)
            result = result + dot(xm[s - 1], weight[theirs, :])
        return result * widen(scale_ref[where, :], result.shape[1])

    h_copies = []

    def keys_values(index):
        where = pl.ds(pl.multiple_of(WINDOW + block_at[index], WINDOW), WINDOW)
        halo[where, 0:k_cols] = finish(index, wk, ak).astype(BF16)
        halo[where, k_cols:] = finish(index, wv, av).astype(BF16)
        if index == 0:
            target, spot = at(z, y, 1 - c), c * (rows + WINDOW)
        else:
            target, spot = (sp + n_sp + 2 * c - 1) % n_sp, (1 - c) * (rows + WINDOW)
        copy = remote(
            halo.at[where],
            halo.at[pl.ds(pl.multiple_of(spot, WINDOW), WINDOW)],
            h_send.at[index], h_recv.at[index], (target, tp),
        )
        copy.start()
        h_copies.append(copy)

    per_head = UNROTATED_WIDTH + D_ROPE
    softmax = per_head ** (-0.5) * LOG2E

    def queries(index):
        where = pl.ds(pl.multiple_of(block_at[index], WINDOW), WINDOW)
        qwin[index] = finish(index, wq, aq).astype(BF16)
        every = finish(index, wlq, alq)
        cosine, sine = cs[0, where, :], cs[1, where, :]
        for h in range(heads):
            one = every[:, h * per_head : (h + 1) * per_head]
            plain = one[:, :UNROTATED_WIDTH].astype(BF16)
            seen = (dot_nt(plain, kup[:, h * UNROTATED_WIDTH : (h + 1) * UNROTATED_WIDTH]) * softmax).astype(BF16)
            turned = turn(one[:, UNROTATED_WIDTH:], cosine, sine) * softmax
            zero = jnp.zeros_like(turned)
            at_rows = slice(h * WINDOW, (h + 1) * WINDOW)
            for v, packed in enumerate(((turned, zero), (zero, turned))):
                qs[v, index, at_rows, 0:UNROTATED_WIDTH] = seen
                qs[v, index, at_rows, UNROTATED_WIDTH:] = jnp.concatenate(packed, axis=1).astype(BF16)

    eye = jnp.where(
        lax.broadcasted_iota(jnp.int32, (UNROTATED_WIDTH, UNROTATED_WIDTH), 0)
        == lax.broadcasted_iota(jnp.int32, (UNROTATED_WIDTH, UNROTATED_WIDTH), 1),
        1.0,
        0.0,
    ).astype(BF16)
    chunk = 4 * rows

    def pieces(d):
        return [(block_of(d, dy, dc), g) for dc in range(2) for dy in range(2) for g in range(parts)]

    def ready(d):
        got_c(d)
        for v in range(2):
            latents = jnp.concatenate(
                [gath[block, g, v * half : (v + 1) * half, :] for block, g in pieces(d)], axis=0
            )
            start = d * chunk + v * (chunk // 2)
            latt[0:UNROTATED_WIDTH, start : start + chunk // 2] = dot_nt(eye, latents).astype(BF16)

    def attend(index, d):
        scores = []
        for v in range(2):
            keys = jnp.concatenate(
                [
                    jnp.concatenate(
                        [gath[block, g, v * half : (v + 1) * half, :], gath[block, g, sub : sub + half, :]], axis=1
                    )
                    for block, g in pieces(d)
                ],
                axis=0,
            )
            scores.append(dot_nt(keys, qs[v, index]))
        new = jnp.maximum(jnp.max(scores[0], axis=0, keepdims=True), jnp.max(scores[1], axis=0, keepdims=True))
        if d > 0:
            old = peaks[index, 0:1]
            new = jnp.maximum(old, new)
        weight = jnp.concatenate([jnp.exp2(part - new).astype(BF16) for part in scores], axis=0)
        added = dot(latt[:, d * chunk : (d + 1) * chunk], weight)
        acct[index] = added if d == 0 else acct[index] * jnp.exp2(old - new) + added
        peaks[index] = jnp.broadcast_to(new, peaks.shape[1:])

    reach = 3 * WINDOW
    seq_total = rows * n_sp

    def window(index):
        start = block_at[index]
        spots = lax.broadcasted_iota(jnp.int32, (WINDOW, reach), 0)
        keys_at = lax.broadcasted_iota(jnp.int32, (WINDOW, reach), 1)
        distance = jnp.abs(spots + WINDOW - keys_at)
        key_pos = sp * rows + start - WINDOW + keys_at
        inside = (distance <= WINDOW) & (key_pos >= 0) & (key_pos < seq_total)
        gone = jnp.where(inside, distance.astype(F32), jnp.inf)
        where = pl.ds(pl.multiple_of(start, WINDOW), reach)
        group = 2
        for kv_head in range(k_cols // DH):
            keys = halo[where, kv_head * DH : (kv_head + 1) * DH]
            values = halo[where, k_cols + kv_head * DH : k_cols + (kv_head + 1) * DH]
            first = kv_head * group
            query = jnp.concatenate(
                [qwin[index, :, (first + j) * DH : (first + j + 1) * DH] for j in range(group)], axis=0
            )
            dots = dot_nt(query, keys) * (DH ** (-0.5) * LOG2E)
            weights, bottoms = [], []
            for j in range(group):
                head = first + j
                place = (tp * sink_ref.shape[0] + head + 1).astype(F32)
                slope = jnp.exp2(jnp.full((1, reach), -8.0 / HEADS_A, F32) * place) * LOG2E
                sink = sink_ref[head] * LOG2E
                scores = dots[j * WINDOW : (j + 1) * WINDOW] - slope * gone
                peak = jnp.maximum(jnp.max(scores, axis=1, keepdims=True), sink)
                weight = jnp.exp2(scores - peak)
                bottoms.append(jnp.sum(weight, axis=1, keepdims=True) + jnp.exp2(sink - peak))
                weights.append(weight.astype(BF16))
            blended = dot(jnp.concatenate(weights, axis=0), values)
            outs = [blended[j * WINDOW : (j + 1) * WINDOW] / bottoms[j] for j in range(group)]
            win[index, :, first * DH : (first + group) * DH] = jnp.concatenate(outs, axis=1).astype(BF16)

    o_copies, f_copies = [], []

    def give(index):
        inverse = 1.0 / acct[index, UNROTATED_WIDTH : UNROTATED_WIDTH + 1, :]
        for h in range(heads):
            where = slice(h * WINDOW, (h + 1) * WINDOW)
            blended = jnp.transpose(acct[index, 0:UNROTATED_WIDTH, where] * inverse[:, where]).astype(BF16)
            spot = slice(h * VALUE_WIDTH, (h + 1) * VALUE_WIDTH)
            lat[index, :, spot] = dot(blended, vup[:, spot]).astype(BF16)

        def terms(j):
            where = pl.ds(pl.multiple_of(j * cols, cols), cols)
            return dot(win[index], ow[:, where]) + dot(lat[index], ol[:, where])

        where = pl.ds(pl.multiple_of(block_at[index], WINDOW), WINDOW)
        for s, other in others:
            outgoing[index, s - 1] = terms(other).astype(BF16)
            copy = remote(
                outgoing.at[index, s - 1], inc_out.at[s - 1, where], o_send.at[index, s], o_recv.at[index, s],
                (sp, other),
            )
            copy.start()
            o_copies.append(copy)
        own[index] = terms(tp)
        copy = pltpu.make_async_copy(own.at[index], own_out.at[where], f_sem.at[index])
        copy.start()
        f_copies.append(copy)

    both = range(parts)
    for g in both:
        got_y(0, g)
        if hi > 1:
            got_z(1, g)
    arrive(0)
    keys_values(0)
    for load in loads[11:]:
        load.wait()
    queries(0)
    ready(0)
    if relayed:
        for g in both:
            got_z(2, g)
        attend(0, 0)
        for g in both:
            got_y(1, g)
            got_z(3, g)
        ready(1)
        attend(0, 1)
        arrive(1)
        keys_values(1)
        for g in both:
            got_y(2, g)
        h_copies[0].wait_recv()
        window(0)
        for g in both:
            got_y(3, g)
        ready(2)
        attend(0, 2)
        ready(3)
        attend(0, 3)
    else:
        attend(0, 0)
        for d in range(1, hi):
            for g in both:
                got_y(d, g)
                if d + 1 < hi:
                    got_z(d + 1, g)
            ready(d)
            attend(0, d)
        arrive(1)
        keys_values(1)
        h_copies[0].wait_recv()
        window(0)
    give(0)
    queries(1)
    for d in range(hi):
        attend(1, d)
    h_copies[1].wait_recv()
    window(1)
    give(1)

    for copy in list(x_copies.values()) + s_copies + list(p_copies.values()) + sends + h_copies:
        copy.wait_send()
    if relayed:

        @pl.when(inner)
        def _():
            for copy in relays:
                copy.wait_send()

    for copy in f_copies + o_copies:
        copy.wait()


def per_device(
    n_sp, n_tp,
    activations, norm_gain, win_query, win_key, win_value, sink_logit, lat_query,
    key_value_down_weight, rope_key, latent_norm_gain, key_up_weight, value_up_weight, out_win, out_lat,
):
    rows, local = activations.shape
    width = local * n_tp
    cols = width // n_tp
    parts = 2
    heads_a = sink_logit.shape[0]
    heads_l = lat_query.shape[1] // (UNROTATED_WIDTH + D_ROPE)
    frequency = 1.0 / ROPE_BASE ** (np.arange(0, D_ROPE, 2) / D_ROPE)
    frequency = np.concatenate([frequency, frequency])[None, :]
    near = np.arange(rows)[:, None] * frequency
    base = (np.arange(n_sp) * rows)[:, None] * frequency
    near = jnp.asarray(np.stack([np.cos(near), np.sin(near)]), F32)
    base = jnp.asarray(np.stack([np.cos(base), np.sin(base)], axis=1), F32)

    smem = pl.BlockSpec(memory_space=pltpu.SMEM)
    hbm = pl.BlockSpec(memory_space=pl.ANY)
    dma = pltpu.SemaphoreType.DMA
    operands = (
        activations, norm_gain.reshape(n_tp, 1, local), near, base, latent_norm_gain.reshape(1, -1),
        key_up_weight, value_up_weight,
        key_value_down_weight, rope_key.T, win_key, win_value, win_query, lat_query, out_win, out_lat,
    )
    order = (0, 1, 2, 3, 4, 5, 6, 7, 8, 9, 10, 11, 12, 13, 14)
    hi = n_sp // 4
    sub = rows // parts
    packed = sub + sub // 2
    blocks = rows // WINDOW
    span = heads_l * WINDOW

    def vmem(shape, kind=BF16):
        return pltpu.VMEM(shape, kind)

    own, incoming = pl.pallas_call(
        functools.partial(layer_kernel, n_sp, n_tp, parts),
        out_shape=(
            jax.ShapeDtypeStruct((rows, cols), F32),
            jax.ShapeDtypeStruct((n_tp - 1, rows, cols), BF16),
        ),
        in_specs=[smem] + [hbm] * len(operands),
        out_specs=(hbm, hbm),
        scratch_shapes=[vmem(operands[i].shape, operands[i].dtype) for i in order]
        + [
            vmem((rows, local)),
            vmem((n_tp - 1, rows, local)),
            vmem((n_tp - 1, WINDOW, local)),
            vmem((rows, win_key.shape[1]), F32),
            vmem((rows, win_value.shape[1]), F32),
            vmem((rows, win_query.shape[1]), F32),
            vmem((rows, lat_query.shape[1]), F32),
            vmem((rows, UNROTATED_WIDTH), F32),
            vmem((rows, D_ROPE), F32),
            vmem((rows, 128), F32),
            vmem((2, rows, D_ROPE), F32),
            vmem((8, rows), F32),
            vmem((n_tp - 1, 8, rows), F32),
            vmem((parts, packed, UNROTATED_WIDTH)),
            vmem((n_tp - 1, parts, packed, UNROTATED_WIDTH)),
            vmem((n_sp, parts, packed, UNROTATED_WIDTH)),
            vmem((UNROTATED_WIDTH + ONES, rows * n_sp)),
            vmem((2, blocks, span, 2 * UNROTATED_WIDTH)),
            vmem((blocks, WINDOW, win_query.shape[1])),
            vmem((rows + 2 * WINDOW, 2 * win_key.shape[1])),
            vmem((blocks, UNROTATED_WIDTH + ONES, span), F32),
            vmem((blocks, 8, span), F32),
            vmem((blocks, WINDOW, heads_a * DH)),
            vmem((blocks, WINDOW, heads_l * VALUE_WIDTH)),
            vmem((blocks, n_tp - 1, WINDOW, cols)),
            vmem((blocks, WINDOW, cols), F32),
            dma((len(operands),)),
            dma((n_tp, 3)), dma((n_tp, 3)),
            dma((n_tp,)), dma((n_tp,)),
            dma((n_tp, parts)), dma((n_tp, parts)),
            dma((hi, parts)), dma((hi, parts)),
            dma((hi, parts)), dma((hi, parts)),
            dma((2 * hi, parts)), dma((2 * hi, parts)),
            dma((2,)), dma((2,)),
            dma((blocks, n_tp)), dma((blocks, n_tp)),
            dma((blocks,)),
        ],
        compiler_params=pltpu.CompilerParams(
            collective_id=0, has_side_effects=True, vmem_limit_bytes=60 * 1024 * 1024
        ),
        name="layer",
    )(sink_logit, *operands)
    total = own
    for s in range(n_tp - 1):
        total = total + incoming[s].astype(F32)
    return total.astype(BF16)


def solution(mesh):
    return jax.shard_map(
        functools.partial(per_device, mesh.shape["sp"], mesh.shape["tp"]),
        mesh=mesh,
        in_specs=(
            P("sp", "tp"),
            P(),
            P(None, "tp"),
            P(None, "tp"),
            P(None, "tp"),
            P("tp"),
            P(None, "tp"),
            P(),
            P(),
            P(),
            P(None, "tp"),
            P(None, "tp"),
            P("tp", None),
            P("tp", None),
        ),
        out_specs=P("sp", "tp"),
        check_vma=False,
    )
```

```python
import functools

import jax
import jax.numpy as jnp
import numpy as np
from jax import lax
from jax.experimental import pallas as pl
from jax.experimental.pallas import tpu as pltpu
from jax.sharding import PartitionSpec as P

HEADS_A = 16
DH = 64
WINDOW = 128
UNROTATED_WIDTH = 128
D_ROPE = 64
VALUE_WIDTH = 128

EPSILON = 1e-06
ROPE_BASE = 10000.0
LOG2E = 1.4426950408889634
MESH = pl.DeviceIdType.MESH
F32 = jnp.float32
BF16 = jnp.bfloat16
ONES = 16


def turn(vectors, cosine, sine):
    half = vectors.shape[-1] // 2
    swapped = jnp.concatenate([vectors[:, half:], vectors[:, :half]], axis=1)
    return vectors * cosine + swapped * sine


def dot_nt(a, b):
    return lax.dot_general(a, b, (((1,), (1,)), ((), ())), preferred_element_type=F32)


def dot(a, b):
    return jnp.dot(a, b, preferred_element_type=F32)


def remote(src, dst, send, recv, device):
    return pltpu.make_async_remote_copy(
        src_ref=src, dst_ref=dst, send_sem=send, recv_sem=recv, device_id=device, device_id_type=MESH
    )


def layer_kernel(
    n_sp, n_tp, parts,
    sink_ref,
    x_hbm, gain_hbm, near_hbm, base_hbm, lng_hbm, kup_hbm, vup_hbm,
    wkv_hbm, wr_hbm, wk_hbm, wv_hbm, wq_hbm, wlq_hbm, ow_hbm, ol_hbm,
    own_out, inc_out,
    xv, gain, near, base, lng, kup, vup, wkv, wr, wk, wv, wq, wlq, ow, ol,
    xn, xr, xm, ak, av, aq, alq, akv, ar, scale_ref, cs, ssq_out, ssq_in, pk_out, pk_in,
    gath, latt, qs, qwin, halo, vt, acct, peaks, win, outgoing, own,
    w_sem, x_send, x_recv, s_send, s_recv, p_send, p_recv, z_send, z_recv, y_send, y_recv,
    c_send, c_recv, h_send, h_recv, o_send, o_recv, f_sem, gate,
):
    sp = lax.axis_index("sp")
    tp = lax.axis_index("tp")
    rows, local = xv.shape
    hi = n_sp // 4
    z, y, c = sp // 4, (sp // 2) % 2, sp % 2
    sub = rows // parts
    half = sub // 2
    heads = acct.shape[2] // WINDOW
    k_cols = ak.shape[1]
    cols = own.shape[2]

    def at(zz, yy, cc):
        return (zz * 2 + yy) * 2 + cc

    others = [(s, (tp + s) % n_tp) for s in range(1, n_tp)]
    sources = [(s, (tp + n_tp - s) % n_tp) for s in range(1, n_tp)]

    pairs = (
        (x_hbm, xv), (wkv_hbm, wkv), (wr_hbm, wr), (gain_hbm, gain),
        (near_hbm, near), (base_hbm, base), (lng_hbm, lng),
        (wk_hbm, wk), (wv_hbm, wv), (wq_hbm, wq), (wlq_hbm, wlq),
        (kup_hbm, kup), (vup_hbm, vup), (ow_hbm, ow), (ol_hbm, ol),
    )
    loads = [pltpu.make_async_copy(a, b, w_sem.at[i]) for i, (a, b) in enumerate(pairs)]
    for load in loads[:4]:
        load.start()

    barrier = pltpu.get_barrier_semaphore()
    late = (sp + n_sp + 2 * c - 1) % n_sp
    across = y == c

    def rank(zz):
        return (zz > 0).astype(jnp.int32) + ((zz > 0) & (zz < hi - 1)).astype(jnp.int32)

    distant = [(None, (z + d) % hi, at((z + d) % hi, y, c)) for d in range(1, hi)]
    distant.append((across, late // 4, late))
    expected, gated, gates = n_tp + 1, 0, []
    for _, other in others:
        pl.semaphore_signal(barrier, inc=1, device_id=(sp, other), device_id_type=MESH)
    for peer in (at(z, 1 - y, c), at(z, y, 1 - c)):
        pl.semaphore_signal(barrier, inc=1, device_id=(peer, tp), device_id_type=MESH)
    for only, zz, peer in distant:
        first, same = rank(z) < rank(zz), rank(z) == rank(zz)
        if only is not None:
            first, same = first & only, same | jnp.logical_not(only)
        last_in = jnp.logical_not(first | same)
        expected = expected + (last_in | same).astype(jnp.int32)
        gated = gated + first.astype(jnp.int32)
        gates.append((last_in, peer))

        @pl.when(first | same)
        def _():
            pl.semaphore_signal(barrier, inc=1, device_id=(peer, tp), device_id_type=MESH)

    for load in loads[4:7]:
        load.start()
    latt[UNROTATED_WIDTH:, :] = jnp.ones_like(latt[UNROTATED_WIDTH:, :])
    for load in loads[:4]:
        load.wait()
    for load in loads[7:]:
        load.start()
    mine = pl.ds(pl.multiple_of(tp * local, local), local)
    wide = xv[...].astype(F32)
    total = jnp.sum(wide * wide, axis=1, keepdims=True)
    ssq_out[...] = jnp.transpose(jnp.broadcast_to(total, (rows, 128)))[0:8]
    xn[...] = (wide * gain[tp]).astype(BF16)
    for g in range(parts):
        span = slice(g * sub, (g + 1) * sub)
        comp = dot(xn[span], wkv[mine, :])
        turned = dot_nt(xn[span], wr[:, mine])
        akv[span] = comp
        ar[span] = turned
        pk_out[g, 0:sub] = comp.astype(BF16)
        pk_out[g, sub:] = jnp.concatenate([turned[:half], turned[half:]], axis=1).astype(BF16)

    pl.semaphore_wait(barrier, expected)
    for last_in, peer in gates:

        @pl.when(last_in)
        def _():
            pl.semaphore_signal(gate, inc=1, device_id=(peer, tp), device_id_type=MESH)

    s_copies = [
        remote(ssq_out, ssq_in.at[s - 1], s_send.at[s], s_recv.at[s], (sp, other)) for s, other in others
    ]
    for copy in s_copies:
        copy.start()
    p_copies = {}
    for g in range(parts):
        for s, other in others:
            p_copies[s, g] = remote(
                pk_out.at[g], pk_in.at[s - 1, g], p_send.at[s, g], p_recv.at[s, g], (sp, other)
            )
            p_copies[s, g].start()

    block_at = [(1 - c) * WINDOW, c * WINDOW]
    x_copies = {}
    for i in range(2):
        where = pl.ds(pl.multiple_of(block_at[i], WINDOW), WINDOW)
        for s, other in others:
            x_copies[s, i] = remote(
                xv.at[where], xr.at[s - 1, where], x_send.at[s, i], x_recv.at[s, i], (sp, other)
            )
            x_copies[s, i].start()

    for load in loads[4:7]:
        load.wait()
    near_cos, near_sin = near[0], near[1]
    base_cos, base_sin = base[sp, 0:1, :], base[sp, 1:2, :]
    plain_sine = near_sin * base_cos + near_cos * base_sin
    lane = lax.broadcasted_iota(jnp.int32, plain_sine.shape, 1)
    cs[0] = near_cos * base_cos - near_sin * base_sin
    cs[1] = jnp.where(lane < D_ROPE // 2, -plain_sine, plain_sine)

    big = ((wk, ak), (wv, av), (wq, aq), (wlq, alq))
    for load, (weight, acc) in zip(loads[7:11], big):
        load.wait()
        acc[...] = dot(xn[...], weight[mine, :])

    relayed = hi == 4
    inner = (z + 1) % 4 >= 2
    if relayed:
        far = 2 - z // 2
        z_of = [z, z + 1 - 2 * (z % 2), far, 3 * (1 - z // 2)]
        z_to = {1: z_of[1], 2: far}
    else:
        z_of = [(z + hi - d) % hi for d in range(hi)]
        z_to = {d: (z + d) % hi for d in range(1, hi)}
    to_y, to_c = (at(z, 1 - y, c), tp), (at(z, y, 1 - c), tp)
    sent = {}

    def block_of(d, dy, dc):
        return at(z_of[d], 1 - y if dy else y, 1 - c if dc else c)

    def own_to_z(d, g):
        part = gath.at[sp, g]
        return remote(part, part, z_send.at[d, g], z_recv.at[z, g], (at(z_to[d], y, c), tp))

    def from_z(d, g):
        part = gath.at[block_of(d, 0, 0), g]
        return remote(part, part, z_send.at[d, g], z_recv.at[z_of[d], g], to_y)

    def relay(d, g):
        part = gath.at[block_of(d, 0, 0), g]
        return remote(part, part, z_send.at[(0, 3)[d - 2], g], z_recv.at[z_of[d], g], (at(z_of[1], y, c), tp))

    def to_row(d, g):
        part = gath.at[block_of(d, 0, 0), g]
        return remote(part, part, y_send.at[d, g], y_recv.at[d, g], to_y)

    def from_row(d, g):
        part = gath.at[block_of(d, 1, 0), g]
        return remote(part, part, y_send.at[d, g], y_recv.at[d, g], to_y)

    def to_core(d, dy, g):
        part, k = gath.at[block_of(d, dy, 0), g], d + hi * dy
        return remote(part, part, c_send.at[k, g], c_recv.at[k, g], to_c)

    def from_core(d, dy, g):
        part, k = gath.at[block_of(d, dy, 1), g], d + hi * dy
        return remote(part, part, c_send.at[k, g], c_recv.at[k, g], to_c)

    def start(make, *spot):
        make(*spot).start()
        sent[(make, *spot)] = functools.partial(make, *spot)

    def got_z(d, g, role=None):
        from_z(d, g).wait_recv()
        if relayed and d >= 2:
            if role is None:
                pl.when(inner)(relay(d, g).start)
            elif role:
                relay(d, g).start()
        start(to_row, d, g)
        start(to_core, d, 0, g)

    def got_y(d, g):
        from_row(d, g).wait_recv()
        start(to_core, d, 1, g)

    def got_c(d):
        for dy in range(2):
            for g in range(parts):
                from_core(d, dy, g).wait_recv()

    for copy in s_copies:
        copy.wait_recv()

    @pl.when(gated > 0)
    def _():
        pl.semaphore_wait(gate, gated)

    total = ssq_out[...]
    for s, _ in sources:
        total = total + ssq_in[s - 1]
    factor = lax.rsqrt(total / (local * n_tp) + EPSILON)
    scale_ref[...] = jnp.transpose(jnp.broadcast_to(factor[0:1], (128, rows)))
    for g in range(parts):
        span = slice(g * sub, (g + 1) * sub)
        comp = akv[span]
        turned = ar[span]
        for s, _ in sources:
            p_copies[s, g].wait_recv()
            comp = comp + pk_in[s - 1, g, 0:sub].astype(F32)
            both = pk_in[s - 1, g, sub:].astype(F32)
            turned = turned + jnp.concatenate([both[:, :D_ROPE], both[:, D_ROPE:]], axis=0)
        latent = comp * lax.rsqrt(jnp.mean(comp * comp, axis=1, keepdims=True) + EPSILON) * lng[...]
        turned = turn(turned * scale_ref[span, 0:D_ROPE], cs[0, span], cs[1, span])
        gath[sp, g, 0:sub] = latent.astype(BF16)
        gath[sp, g, sub:] = jnp.concatenate([turned[:half], turned[half:]], axis=1).astype(BF16)
        for d in reversed(z_to):
            start(own_to_z, d, g)
        start(to_row, 0, g)
        start(to_core, 0, 0, g)

    def widen(scale, width):
        return jnp.concatenate([scale] * (-(-width // 128)), axis=1)[:, :width]

    def arrive(index):
        for s, _ in others:
            x_copies[s, index].wait_recv()
        where = pl.ds(pl.multiple_of(block_at[index], WINDOW), WINDOW)
        for s, source in sources:
            xm[s - 1] = (xr[s - 1, where, :].astype(F32) * gain[source]).astype(BF16)

    def finish(index, weight, acc):
        where = pl.ds(pl.multiple_of(block_at[index], WINDOW), WINDOW)
        result = acc[where, :]
        for s, source in sources:
            theirs = pl.ds(pl.multiple_of(source * local, local), local)
            result = result + dot(xm[s - 1], weight[theirs, :])
        return result * widen(scale_ref[where, :], result.shape[1])

    h_copies = []

    def keys_values(index):
        where = pl.ds(pl.multiple_of(WINDOW + block_at[index], WINDOW), WINDOW)
        halo[where, 0:k_cols] = finish(index, wk, ak).astype(BF16)
        halo[where, k_cols:] = finish(index, wv, av).astype(BF16)
        if index == 0:
            target, spot = at(z, y, 1 - c), c * (rows + WINDOW)
        else:
            target, spot = late, (1 - c) * (rows + WINDOW)
        copy = remote(
            halo.at[where],
            halo.at[pl.ds(pl.multiple_of(spot, WINDOW), WINDOW)],
            h_send.at[index], h_recv.at[index], (target, tp),
        )
        copy.start()
        h_copies.append(copy)
        flip(WINDOW + block_at[index])

    per_head = UNROTATED_WIDTH + D_ROPE
    softmax = per_head ** (-0.5) * LOG2E

    def queries(index):
        where = pl.ds(pl.multiple_of(block_at[index], WINDOW), WINDOW)
        qwin[index] = finish(index, wq, aq).astype(BF16)
        every = finish(index, wlq, alq)
        cosine, sine = cs[0, where, :], cs[1, where, :]
        ones_of = [every[:, h * per_head : (h + 1) * per_head] for h in range(heads)]
        seen = [
            dot_nt(ones_of[h][:, :UNROTATED_WIDTH].astype(BF16), kup[:, h * UNROTATED_WIDTH : (h + 1) * UNROTATED_WIDTH])
            for h in range(heads)
        ]
        for h in range(heads):
            turned = turn(ones_of[h][:, UNROTATED_WIDTH:], cosine, sine) * softmax
            zero = jnp.zeros_like(turned)
            at_rows = slice(h * WINDOW, (h + 1) * WINDOW)
            plain = (seen[h] * softmax).astype(BF16)
            for v, packed in enumerate(((turned, zero), (zero, turned))):
                qs[v, index, at_rows, 0:UNROTATED_WIDTH] = plain
                qs[v, index, at_rows, UNROTATED_WIDTH:] = jnp.concatenate(packed, axis=1).astype(BF16)

    eye = jnp.where(
        lax.broadcasted_iota(jnp.int32, (UNROTATED_WIDTH, UNROTATED_WIDTH), 0)
        == lax.broadcasted_iota(jnp.int32, (UNROTATED_WIDTH, UNROTATED_WIDTH), 1),
        1.0,
        0.0,
    ).astype(BF16)
    chunk = 4 * rows

    def pieces(d):
        return [(block_of(d, dy, dc), g) for dc in range(2) for dy in range(2) for g in range(parts)]

    def ready(d):
        got_c(d)
        for v in range(2):
            latents = jnp.concatenate(
                [gath[block, g, v * half : (v + 1) * half, :] for block, g in pieces(d)], axis=0
            )
            start = d * chunk + v * (chunk // 2)
            latt[0:UNROTATED_WIDTH, start : start + chunk // 2] = dot_nt(eye, latents).astype(BF16)

    tile = min(2 * WINDOW, heads * WINDOW)

    def scores_of(index, d, t):
        found = []
        for v in range(2):
            keys = jnp.concatenate(
                [
                    jnp.concatenate(
                        [gath[block, g, v * half : (v + 1) * half, :], gath[block, g, sub : sub + half, :]], axis=1
                    )
                    for block, g in pieces(d)
                ],
                axis=0,
            )
            found.append(dot_nt(keys, qs[v, index, t * tile : (t + 1) * tile, :]))
        return found

    def attend(*steps):
        units = [(index, d, t) for index, d in steps for t in range(heads * WINDOW // tile)]
        later = scores_of(*units[0])
        held = None

        def blend(index, d, span, weight, old, new):
            added = dot(latt[:, d * chunk : (d + 1) * chunk], weight)
            acct[index, :, span] = added if d == 0 else acct[index, :, span] * jnp.exp2(old - new) + added

        for i, (index, d, t) in enumerate(units):
            scores = later
            if i + 1 < len(units):
                later = scores_of(*units[i + 1])
            span = slice(t * tile, (t + 1) * tile)
            new = jnp.maximum(jnp.max(scores[0], axis=0, keepdims=True), jnp.max(scores[1], axis=0, keepdims=True))
            old = None
            if d > 0:
                old = peaks[index, 0:1, span]
                new = jnp.maximum(old, new)
            peaks[index, 0:1, span] = new
            weight = jnp.concatenate([jnp.exp2(part - new).astype(BF16) for part in scores], axis=0)
            if held:
                blend(*held)
            held = (index, d, span, weight, old, new)
        blend(*held)

    reach = 3 * WINDOW
    seq_total = rows * n_sp
    square = jnp.where(
        lax.broadcasted_iota(jnp.int32, (k_cols, k_cols), 0) == lax.broadcasted_iota(jnp.int32, (k_cols, k_cols), 1),
        1.0,
        0.0,
    ).astype(BF16)

    def flip(spot):
        where = pl.ds(pl.multiple_of(spot, WINDOW), WINDOW)
        vt[:, where] = dot_nt(square, halo[where, k_cols:]).astype(BF16)

    def window(index):
        h_copies[index].wait_recv()
        flip((1 - c if index == 0 else c) * (rows + WINDOW))
        start_at = block_at[index]
        keys_at = lax.broadcasted_iota(jnp.int32, (reach, WINDOW), 0)
        spots = lax.broadcasted_iota(jnp.int32, (reach, WINDOW), 1)
        distance = jnp.abs(spots + WINDOW - keys_at)
        key_pos = sp * rows + start_at - WINDOW + keys_at
        inside = (distance <= WINDOW) & (key_pos >= 0) & (key_pos < seq_total)
        gone = jnp.where(inside, distance.astype(F32), jnp.inf)
        where = pl.ds(pl.multiple_of(start_at, WINDOW), reach)
        ones = jnp.ones((ONES, reach), BF16)
        group = 2
        kv_heads = range(k_cols // DH)
        own_cols = [slice(kv_head * DH, (kv_head + 1) * DH) for kv_head in kv_heads]
        dots = []
        for kv_head in kv_heads:
            query = jnp.concatenate(
                [qwin[index, :, n * DH : (n + 1) * DH] for n in range(kv_head * group, (kv_head + 1) * group)], axis=0
            )
            dots.append(dot_nt(halo[where, own_cols[kv_head]], query))
        weights, sinks = [], []
        for kv_head in kv_heads:
            for j in range(group):
                head = kv_head * group + j
                place = (tp * sink_ref.shape[0] + head + 1).astype(F32)
                slope = jnp.exp2(jnp.full((1, WINDOW), -8.0 / HEADS_A, F32) * place) * LOG2E
                sink = sink_ref[head] * LOG2E
                scores = dots[kv_head][:, j * WINDOW : (j + 1) * WINDOW] * (DH ** (-0.5) * LOG2E) - slope * gone
                peak = jnp.maximum(jnp.max(scores, axis=0, keepdims=True), sink)
                weights.append(jnp.exp2(scores - peak).astype(BF16))
                sinks.append(jnp.exp2(sink - peak))
        blends = []
        for kv_head in kv_heads:
            mine_of = slice(kv_head * group, (kv_head + 1) * group)
            left_side = jnp.concatenate([vt[own_cols[kv_head], where], ones], axis=0)
            blends.append(dot(left_side, jnp.concatenate(weights[mine_of], axis=1)))
        for kv_head in kv_heads:
            bottom = blends[kv_head][DH : DH + 1] + jnp.concatenate(
                sinks[kv_head * group : (kv_head + 1) * group], axis=1
            )
            blended = blends[kv_head][0:DH] / bottom
            pair = jnp.concatenate([blended[:, j * WINDOW : (j + 1) * WINDOW] for j in range(group)], axis=0)
            first = kv_head * group
            win[index, :, first * DH : (first + group) * DH] = jnp.transpose(pair).astype(BF16)

    o_copies, f_copies = [], []

    def give(index):
        inverse = 1.0 / acct[index, UNROTATED_WIDTH : UNROTATED_WIDTH + 1, :]
        flipped = []
        for h in range(heads):
            where = slice(h * WINDOW, (h + 1) * WINDOW)
            flipped.append(jnp.transpose(acct[index, 0:UNROTATED_WIDTH, where] * inverse[:, where]).astype(BF16))
        lats = jnp.concatenate(
            [dot(flipped[h], vup[:, h * VALUE_WIDTH : (h + 1) * VALUE_WIDTH]).astype(BF16) for h in range(heads)],
            axis=1,
        )
        wins = win[index]

        def terms(j):
            where = pl.ds(pl.multiple_of(j * cols, cols), cols)
            return dot(wins, ow[:, where]) + dot(lats, ol[:, where])

        where = pl.ds(pl.multiple_of(block_at[index], WINDOW), WINDOW)
        for s, other in others:
            outgoing[index, s - 1] = terms(other).astype(BF16)
            copy = remote(
                outgoing.at[index, s - 1], inc_out.at[s - 1, where], o_send.at[index, s], o_recv.at[index, s],
                (sp, other),
            )
            copy.start()
            o_copies.append(copy)
        own[index] = terms(tp)
        copy = pltpu.make_async_copy(own.at[index], own_out.at[where], f_sem.at[index])
        copy.start()
        f_copies.append(copy)

    both = range(parts)
    last = hi - 1

    def events(*todo):
        for got, d in todo:
            for g in both:
                got(d, g)

    def on(role, todo):
        @pl.when(inner if role else jnp.logical_not(inner))
        def _():
            for got, d in todo:
                for g in both:
                    if got is got_z:
                        got_z(d, g, role)
                    else:
                        got(d, g)

    def inside_z(*todo):
        on(True, todo)

    def outside_z(*todo):
        on(False, todo)

    if relayed:
        for g in both:
            got_y(0, g)
            got_z(1, g)
        inside_z((got_z, 2), (got_z, 3))
        ready(0)
        arrive(0)
        keys_values(0)
        inside_z((got_y, 1))
        for load in loads[11:]:
            load.wait()
        queries(0)
        attend((0, 0))
        inside_z((got_y, 2))
        outside_z((got_y, 1), (got_z, 2))
        ready(1)
        attend((0, 1))
        inside_z((got_y, 3))
        outside_z((got_z, 3))
        arrive(1)
        keys_values(1)
        outside_z((got_y, 2))
        window(0)
        queries(1)
        ready(2)
        outside_z((got_y, 3))
        attend((0, 2))
    else:
        for d in range(1, hi):
            events((got_y, d - 1), (got_z, d))
        events((got_y, last))
        arrive(0)
        keys_values(0)
        for load in loads[11:]:
            load.wait()
        queries(0)
        for d in range(last - 1):
            ready(d)
            attend((0, d))
        ready(last - 1)
        arrive(1)
        keys_values(1)
        window(0)
        queries(1)
        attend((0, last - 1))
    ready(last)
    attend((0, last))
    give(0)
    window(1)
    attend(*[(1, d) for d in range(hi)])
    give(1)

    for copy in list(x_copies.values()) + s_copies + list(p_copies.values()) + h_copies:
        copy.wait_send()
    for make in sent.values():
        make().wait_send()
    if relayed:

        @pl.when(inner)
        def _():
            for d in (2, 3):
                for g in both:
                    relay(d, g).wait_send()

    for copy in f_copies + o_copies:
        copy.wait()


def per_device(
    n_sp, n_tp,
    activations, norm_gain, win_query, win_key, win_value, sink_logit, lat_query,
    key_value_down_weight, rope_key, latent_norm_gain, key_up_weight, value_up_weight, out_win, out_lat,
):
    rows, local = activations.shape
    width = local * n_tp
    cols = width // n_tp
    parts = 2
    heads_a = sink_logit.shape[0]
    heads_l = lat_query.shape[1] // (UNROTATED_WIDTH + D_ROPE)
    frequency = 1.0 / ROPE_BASE ** (np.arange(0, D_ROPE, 2) / D_ROPE)
    frequency = np.concatenate([frequency, frequency])[None, :]
    near = np.arange(rows)[:, None] * frequency
    base = (np.arange(n_sp) * rows)[:, None] * frequency
    near = jnp.asarray(np.stack([np.cos(near), np.sin(near)]), F32)
    base = jnp.asarray(np.stack([np.cos(base), np.sin(base)], axis=1), F32)

    smem = pl.BlockSpec(memory_space=pltpu.SMEM)
    hbm = pl.BlockSpec(memory_space=pl.ANY)
    dma = pltpu.SemaphoreType.DMA
    operands = (
        activations, norm_gain.reshape(n_tp, 1, local), near, base, latent_norm_gain.reshape(1, -1),
        key_up_weight, value_up_weight,
        key_value_down_weight, rope_key.T, win_key, win_value, win_query, lat_query, out_win, out_lat,
    )
    order = (0, 1, 2, 3, 4, 5, 6, 7, 8, 9, 10, 11, 12, 13, 14)
    hi = n_sp // 4
    sub = rows // parts
    packed = sub + sub // 2
    blocks = rows // WINDOW
    span = heads_l * WINDOW

    def vmem(shape, kind=BF16):
        return pltpu.VMEM(shape, kind)

    own, incoming = pl.pallas_call(
        functools.partial(layer_kernel, n_sp, n_tp, parts),
        out_shape=(
            jax.ShapeDtypeStruct((rows, cols), F32),
            jax.ShapeDtypeStruct((n_tp - 1, rows, cols), BF16),
        ),
        in_specs=[smem] + [hbm] * len(operands),
        out_specs=(hbm, hbm),
        scratch_shapes=[vmem(operands[i].shape, operands[i].dtype) for i in order]
        + [
            vmem((rows, local)),
            vmem((n_tp - 1, rows, local)),
            vmem((n_tp - 1, WINDOW, local)),
            vmem((rows, win_key.shape[1]), F32),
            vmem((rows, win_value.shape[1]), F32),
            vmem((rows, win_query.shape[1]), F32),
            vmem((rows, lat_query.shape[1]), F32),
            vmem((rows, UNROTATED_WIDTH), F32),
            vmem((rows, D_ROPE), F32),
            vmem((rows, 128), F32),
            vmem((2, rows, D_ROPE), F32),
            vmem((8, rows), F32),
            vmem((n_tp - 1, 8, rows), F32),
            vmem((parts, packed, UNROTATED_WIDTH)),
            vmem((n_tp - 1, parts, packed, UNROTATED_WIDTH)),
            vmem((n_sp, parts, packed, UNROTATED_WIDTH)),
            vmem((UNROTATED_WIDTH + ONES, rows * n_sp)),
            vmem((2, blocks, span, 2 * UNROTATED_WIDTH)),
            vmem((blocks, WINDOW, win_query.shape[1])),
            vmem((rows + 2 * WINDOW, 2 * win_key.shape[1])),
            vmem((win_key.shape[1], rows + 2 * WINDOW)),
            vmem((blocks, UNROTATED_WIDTH + ONES, span), F32),
            vmem((blocks, 8, span), F32),
            vmem((blocks, WINDOW, heads_a * DH)),
            vmem((blocks, n_tp - 1, WINDOW, cols)),
            vmem((blocks, WINDOW, cols), F32),
            dma((len(operands),)),
            dma((n_tp, 2)), dma((n_tp, 2)),
            dma((n_tp,)), dma((n_tp,)),
            dma((n_tp, parts)), dma((n_tp, parts)),
            dma((hi, parts)), dma((hi, parts)),
            dma((hi, parts)), dma((hi, parts)),
            dma((2 * hi, parts)), dma((2 * hi, parts)),
            dma((2,)), dma((2,)),
            dma((blocks, n_tp)), dma((blocks, n_tp)),
            dma((blocks,)),
            pltpu.SemaphoreType.REGULAR,
        ],
        compiler_params=pltpu.CompilerParams(
            collective_id=0, has_side_effects=True, vmem_limit_bytes=60 * 1024 * 1024
        ),
        name="layer",
    )(sink_logit, *operands)
    total = own
    for s in range(n_tp - 1):
        total = total + incoming[s].astype(F32)
    return total.astype(BF16)


def solution(mesh):
    return jax.shard_map(
        functools.partial(per_device, mesh.shape["sp"], mesh.shape["tp"]),
        mesh=mesh,
        in_specs=(
            P("sp", "tp"),
            P(),
            P(None, "tp"),
            P(None, "tp"),
            P(None, "tp"),
            P("tp"),
            P(None, "tp"),
            P(),
            P(),
            P(),
            P(None, "tp"),
            P(None, "tp"),
            P("tp", None),
            P("tp", None),
        ),
        out_specs=P("sp", "tp"),
        check_vma=False,
    )
```
